32 devices in a mesh: sp: 4 (over z), fs: 4 (over y, x), tp: 2 (over core).
Axes of the slice: x: 2, y: 2, z: 4, core: 2. Of those that a mesh axis runs over, the one named last changes fastest.
Arguments:
- tokens: bfloat16 [2048, 2048], P(('fs', 'sp')), may hold values from -6 to 6
- in_gain: float32 [2048], replicated, may hold values from 0.1 to 1.9
- query_weight: bfloat16 [2048, 512], P(None, ('tp', 'fs')), may hold values from -0.17291713 to 0.17291713
- key_weight: bfloat16 [2048, 512], P(None, ('tp', 'fs')), may hold values from -0.17291713 to 0.17291713
- value_weight: bfloat16 [2048, 512], P(None, ('tp', 'fs')), may hold values from -0.125 to 0.125
- rec_query_weight: bfloat16 [2048, 512], P(None, ('tp', 'fs')), may hold values from -0.125 to 0.125
- rec_forget_weight: bfloat16 [2048, 512], P(None, ('tp', 'fs')), may hold values from -0.125 to 0.125
- rec_input_weight: bfloat16 [2048, 512], P(None, ('tp', 'fs')), may hold values from -0.125 to 0.125
- mix_lambda: float32 [4], P('tp'), may hold values from 0.3 to 0.8
- lower_bound: float32 [4, 128], P('tp'), may hold values from 0.9 to 0.9995117
- forget_scale: float32 [2048], P(('fs', 'sp')), may hold values from 0.35 to 1536
- att_gain: float32 [128], replicated, may hold values from 0.1 to 1.9
- recurrence_gain: float32 [128], replicated, may hold values from 0.1 to 1.9
- att_out_weight: bfloat16 [512, 2048], P('tp'), may hold values from -0.1875 to 0.1875
- rec_out_weight: bfloat16 [512, 2048], P('tp'), may hold values from -0.1875 to 0.1875
Outputs:
- mixed_out: bfloat16 [2048, 2048], P(('fs', 'sp'))
- log_weight_sum: float32 [4, 2048], P('tp', ('fs', 'sp'))
The draws below stay inside these ranges and needn't reach their ends.
All inputs are finite; a program needn't handle non-finite values.
Results may differ from the reference program's by a relative error of at most 0.012.
Values may be sent and summed in bfloat16 or wider, within the bound.
A program may use at most 128 MiB of HBM per device.

```python
import math
import jax
import jax.numpy as jnp
from jax import lax

D = 2048
HEADS = 4
DK = 64
DV = 128
BLK = 64
TOK_DEV = 128
LENGTH_PER_SEQ = 512
SEQS = 4
TOKEN_COUNT_ALL = 2048
N_TP = 2


def drawn_weight(key, salt):
    spread = (D * 10 // 17) ** (-0.5)
    noise = jnp.clip(jax.random.normal(jax.random.fold_in(key, salt), (D, HEADS * 2 * DK), jnp.float32), -4.5, 4.5) * spread
    return jnp.clip(noise, -6.0 * spread, 6.0 * spread).astype(jnp.bfloat16)


def draw_tokens(key, part):
    base = jax.random.normal(jax.random.fold_in(key, 41), (TOKEN_COUNT_ALL, D), jnp.float32)
    return jnp.clip(base, -6.0, 6.0).astype(jnp.bfloat16)


def draw_query_weight(key, part):
    return drawn_weight(key, 51)


def draw_key_weight(key, part):
    return drawn_weight(key, 53)


def draw_lower_bound(key, part):
    first_key, second_key = jax.random.split(jax.random.fold_in(key, 11))
    slower = jax.random.uniform(first_key, (HEADS, DV), jnp.float32) < 0.5
    mixing = jax.random.uniform(second_key, (HEADS, DV), jnp.float32)
    slower_minimum = 0.25 / LENGTH_PER_SEQ
    slow_gap = jnp.exp(math.log(slower_minimum) + mixing * math.log(3.0))
    fast_gap = jnp.exp(math.log(0.04) + mixing * (math.log(0.1) - math.log(0.04)))
    return (1.0 - jnp.where(slower, slow_gap, fast_gap)).astype(jnp.float32)


def draw_forget_scale(key, part):
    key_collection = jax.random.split(jax.random.fold_in(key, 23), 4)
    device_factor = jnp.exp(math.log(0.5) + jax.random.uniform(key_collection[0], (TOKEN_COUNT_ALL // TOK_DEV,), jnp.float32) * math.log(4.0))
    block_factor = jnp.exp(jax.random.uniform(key_collection[1], (TOKEN_COUNT_ALL // BLK,), jnp.float32) * 0.6 - 0.3)
    initial_scale = jnp.repeat(device_factor, TOK_DEV) * jnp.repeat(block_factor, BLK)
    sudden_rows = jax.random.uniform(key_collection[2], (TOKEN_COUNT_ALL,), jnp.float32) < 2.5 / LENGTH_PER_SEQ
    height_per_level = LENGTH_PER_SEQ * (1.0 + 2.0 * jax.random.uniform(key_collection[3], (TOKEN_COUNT_ALL,), jnp.float32))
    return jnp.where(sudden_rows, height_per_level, initial_scale).astype(jnp.float32)


def shard_levels(rng, shape, cuts, least, largest):
    factor_of = 1.0
    for axis_at, shards_of in cuts:
        heights = jax.random.uniform(jax.random.fold_in(jax.random.fold_in(rng, 6), axis_at), (shards_of,), jnp.float32, least / len(cuts), largest / len(cuts))
        factor_of = factor_of * jnp.repeat(jnp.exp(heights), shape[axis_at] // shards_of).reshape((-1,) + (1,) * (len(shape) - 1 - axis_at))
    return factor_of


def bell_draw(rng, extent, scale, reach, cuts=(), kind=jnp.bfloat16):
    values = jax.random.normal(rng, extent, jnp.float32) * scale
    if len(cuts) > 0:
        values = shard_levels(rng, extent, cuts, -0.22, 0.18) * values
    return jnp.clip(values, min=-reach, max=reach).astype(kind)


def setup_inputs(seed: int = 0) -> dict:
    key_of = jax.random.split(jax.random.key(seed), 16)
    return {
        "tokens": draw_tokens(jax.random.fold_in(key_of[15], 71), 0),
        "in_gain": jnp.clip(1.0 + 0.18 * jax.random.normal(key_of[1], (D,), jnp.float32), 0.1, 1.9),
        "query_weight": draw_query_weight(jax.random.fold_in(key_of[15], 71), 0),
        "key_weight": draw_key_weight(jax.random.fold_in(key_of[15], 71), 0),
        "value_weight": bell_draw(key_of[4], (D, HEADS * DV), D ** -0.5, 0.125, ((1, 8),)),
        "rec_query_weight": bell_draw(key_of[5], (D, HEADS * DV), D ** -0.5, 0.125, ((1, 8),)),
        "rec_forget_weight": bell_draw(key_of[6], (D, HEADS * DV), D ** -0.5, 0.125, ((1, 8),)),
        "rec_input_weight": bell_draw(key_of[7], (D, HEADS * DV), D ** -0.5, 0.125, ((1, 8),)),
        "mix_lambda": jnp.clip(0.3 + 0.5 * jax.random.uniform(key_of[8], (HEADS,), jnp.float32) ** shard_levels(key_of[8], (HEADS,), ((0, 2),), -0.2, 0.2), 0.3, 0.8),
        "lower_bound": draw_lower_bound(jax.random.fold_in(key_of[15], 71), 0),
        "forget_scale": draw_forget_scale(jax.random.fold_in(key_of[15], 71), 0),
        "att_gain": jnp.clip(1.0 + 0.18 * jax.random.normal(key_of[11], (DV,), jnp.float32), 0.1, 1.9),
        "recurrence_gain": jnp.clip(1.0 + 0.18 * jax.random.normal(key_of[12], (DV,), jnp.float32), 0.1, 1.9),
        "att_out_weight": bell_draw(key_of[13], (HEADS * DV, D), (2 * HEADS * DV) ** -0.5, 0.1875, ((0, 2),)),
        "rec_out_weight": bell_draw(key_of[14], (HEADS * DV, D), (2 * HEADS * DV) ** -0.5, 0.1875, ((0, 2),)),
    }


EPS = 1e-06
NEG = -1e+30
QUERY_ROWS = 512

def norm_rows(values, gain):
    return values * lax.rsqrt(lax.optimization_barrier(jnp.mean(values * values, axis=-1, keepdims=True)) + EPS) * gain

def to_sequences(rows):
    return rows.reshape(SEQS, LENGTH_PER_SEQ, rows.shape[-1])

def from_sequences(seq_rows):
    return seq_rows.reshape(TOKEN_COUNT_ALL, seq_rows.shape[-1])

def block_recurrence(queries, key_in, value_in, log_forget):
    head_count, row_count, key_width = queries.shape
    block_count = row_count // BLK

    def to_blocks(array_in):
        return array_in.reshape(head_count, block_count, BLK, array_in.shape[-1]).transpose(1, 0, 2, 3)
    causal = jnp.tril(jnp.ones((BLK, BLK), bool))

    def advance(passed_state, inputs):
        query_block, key_block, value_block, l_blk = inputs
        accumulator_sum = jnp.cumsum(l_blk, axis=1)
        cross_block_output = jnp.einsum('sre,sei->sri', query_block * jnp.exp(accumulator_sum), passed_state, precision=lax.Precision.HIGHEST)
        spread = accumulator_sum[:, :, None, :] - accumulator_sum[:, None, :, :]
        decay = jnp.exp(jnp.where(causal[None, :, :, None], spread, -jnp.inf))
        scores = jnp.einsum('htk,htsk,hsk->hts', query_block, decay, key_block, precision=lax.Precision.HIGHEST)
        result = cross_block_output + jnp.einsum('hts,hsv->htv', scores, value_block, precision=lax.Precision.HIGHEST)
        final_log_sum = accumulator_sum[:, -1:, :]
        updated_state = jnp.exp(final_log_sum[:, 0, :])[:, :, None] * passed_state + jnp.einsum('plf,plt->pft', key_block * jnp.exp(final_log_sum - accumulator_sum), value_block, precision=lax.Precision.HIGHEST)
        return (updated_state, result)
    begin_state = jnp.zeros((head_count, key_width, value_in.shape[-1]), jnp.float32)
    end_state, results = lax.scan(advance, begin_state, (to_blocks(queries), to_blocks(key_in), to_blocks(value_in), to_blocks(log_forget)))
    return (end_state, results.transpose(1, 0, 2, 3).reshape(head_count, row_count, value_in.shape[-1]))

def attend_sequence(q_seq, k_seq, v_seq, mix_lambda, att_gain):
    length_now = q_seq.shape[0]
    queries = q_seq.reshape(length_now, HEADS, 2, DK).transpose(1, 2, 0, 3).astype(jnp.float32)
    key_heads = k_seq.reshape(length_now, HEADS, 2, DK).transpose(1, 2, 0, 3).astype(jnp.float32)
    head_values = v_seq.reshape(length_now, HEADS, DV).transpose(1, 0, 2).astype(jnp.float32)
    block_rows = min(QUERY_ROWS, length_now)
    key_pos = jnp.arange(length_now, dtype=jnp.int32)

    def one_block(block_index):
        begin_row = (block_index * block_rows).astype(jnp.int32)
        query_block = lax.dynamic_slice_in_dim(queries, begin_row, block_rows, 2)
        q_pos = begin_row + jnp.arange(block_rows, dtype=jnp.int32)
        allowed = q_pos[:, None] >= key_pos[None, :]
        scores = jnp.einsum('hmqd,hmkd->hmqk', query_block, key_heads) * DK ** (-0.5)
        scores = jnp.where(allowed, scores, NEG)
        highest = lax.optimization_barrier(jnp.max(scores, axis=-1))
        weights = jnp.exp(scores - highest[..., None])
        weight_sum = lax.optimization_barrier(jnp.sum(weights, axis=-1))
        rounded_weights = lax.optimization_barrier(weights.astype(jnp.bfloat16)).astype(jnp.float32)
        summed_values = jnp.einsum('itap,ipn->itan', rounded_weights, head_values)
        mixed = summed_values[:, 0] / weight_sum[:, 0, :, None] - mix_lambda[:, None, None] * summed_values[:, 1] / weight_sum[:, 1, :, None]
        result = (norm_rows(mixed, att_gain) * 0.8).astype(jnp.bfloat16)
        return (result.transpose(1, 0, 2).reshape(block_rows, HEADS * DV), highest[:, 0] + jnp.log(weight_sum[:, 0]))
    results, log_sums = lax.map(one_block, jnp.arange(length_now // block_rows, dtype=jnp.int32))
    return (results.reshape(length_now, HEADS * DV), log_sums.transpose(1, 0, 2).reshape(HEADS, length_now))

def recur_sequence(rq_seq, rf_seq, ri_seq, scale_seq, lower_bound, recurrence_gain):
    length_now = rq_seq.shape[0]

    def heads_first(array_in):
        return array_in.reshape(length_now, HEADS, DV).transpose(1, 0, 2).astype(jnp.float32)
    queries = heads_first(rq_seq)
    lower_edge = lower_bound[:, None, :]
    forget = lower_edge + (1.0 - lower_edge) * jax.nn.sigmoid(heads_first(rf_seq))
    log_forget = scale_seq[None, :, None] * jnp.log(forget)
    key_in = 1.0 - jnp.exp(log_forget)
    _, results = block_recurrence(queries, key_in, heads_first(ri_seq), log_forget)
    normed_out = norm_rows(results, recurrence_gain).astype(jnp.bfloat16)
    return normed_out.transpose(1, 0, 2).reshape(length_now, HEADS * DV)

def reference(tokens, in_gain, query_weight, key_weight, value_weight, rec_query_weight, rec_forget_weight, rec_input_weight, mix_lambda, lower_bound, forget_scale, att_gain, recurrence_gain, att_out_weight, rec_out_weight):
    normed = norm_rows(tokens.astype(jnp.float32), in_gain).astype(jnp.bfloat16)

    def project(weight):
        return to_sequences(jnp.dot(normed, weight, preferred_element_type=jnp.float32).astype(jnp.bfloat16))
    pieces = tuple((project(weight) for weight in (query_weight, key_weight, value_weight, rec_query_weight, rec_forget_weight, rec_input_weight)))
    scales = to_sequences(forget_scale[:, None])[:, :, 0]

    def per_sequence(inputs):
        q_seq, k_seq, v_seq, rq_seq, rf_seq, ri_seq, scale_seq = inputs
        att_rows, log_sums = attend_sequence(q_seq, k_seq, v_seq, mix_lambda, att_gain)
        rec_rows = recur_sequence(rq_seq, rf_seq, ri_seq, scale_seq, lower_bound, recurrence_gain)
        return (att_rows, rec_rows, log_sums)
    att_all, rec_all, log_all = lax.map(per_sequence, pieces + (scales,))
    att_all = from_sequences(att_all)
    rec_all = from_sequences(rec_all)
    log_weight_sum = from_sequences(log_all.transpose(0, 2, 1)).transpose(1, 0)
    group_width = HEADS * DV // N_TP
    mixed = jnp.zeros((TOKEN_COUNT_ALL, D), jnp.float32)
    for group in range(N_TP):
        lower_col = group * group_width
        upper_col = lower_col + group_width
        portion = jnp.dot(att_all[:, lower_col:upper_col], att_out_weight[lower_col:upper_col], preferred_element_type=jnp.float32)
        portion = portion + jnp.dot(rec_all[:, lower_col:upper_col], rec_out_weight[lower_col:upper_col], preferred_element_type=jnp.float32)
        mixed = mixed + lax.optimization_barrier(portion.astype(jnp.bfloat16)).astype(jnp.float32)
    return (mixed.astype(jnp.bfloat16), log_weight_sum)
```

```python
import functools

import jax
import jax.numpy as jnp
from jax import lax
from jax.experimental import pallas as pl
from jax.experimental.pallas import tpu as pltpu
from jax.sharding import PartitionSpec as P

DK = 64
DV = 128
SUB = 16
EPS = 1e-06
NEG = -1e30
MESH = pl.DeviceIdType.MESH


def dot_nt(a, b):
    return lax.dot_general(a, b, (((1,), (1,)), ((), ())), preferred_element_type=jnp.float32)


def dot_nn(a, b):
    return jnp.dot(a, b, preferred_element_type=jnp.float32)


def partner(f, d, n, sign):
    if n & (n - 1):
        return lax.rem(f + sign * d + n, n)
    out, bit = 0, 1
    while bit < n:
        mine = lax.rem(f // bit, 2)
        out = out + bit * ((1 - mine) if d & bit else mine)
        bit *= 2
    return out


def kernel(
    n_sp, n_fs, n_tp, st_dtype,
    tok, gain, w0, w1, w2, w3, w4, w5, lam, lower, scale, att_gain, rec_gain, aow, row_w,
    mixed, lse,
    wv, aov, rov, wcat, tok_all, nrm, psend, osend, kvall, pr, oprecv, part,
    smat, olocal, qdec, send_st, s_in, s_out, m_s, l_s, acc,
    w_sem, o_sem, tok_s, tok_r, rel_s, rel_r, a_s, a_r, b_s, b_r, kv_s, kv_r, st_s, st_r, op_s, op_r,
):
    z, f, t = lax.axis_index("sp"), lax.axis_index("fs"), lax.axis_index("tp")
    rows, width = tok.shape
    half = rows // n_tp
    heads = n_fs // 2
    nxt, prv = lax.rem(z + 1, n_sp), lax.rem(z + n_sp - 1, n_sp)

    wcopies = [
        pltpu.make_async_copy(w, wv.at[i], w_sem.at[i])
        for i, w in enumerate((w0, w1, w2, w3, w4, w5))
    ]
    for c in wcopies:
        c.start()
    ocopies = [
        pltpu.make_async_copy(aow, aov, o_sem.at[0]),
        pltpu.make_async_copy(row_w, rov, o_sem.at[1]),
    ]

    barrier = pltpu.get_barrier_semaphore()
    for d in range(1, n_fs):
        pl.semaphore_signal(barrier, inc=1, device_id={"fs": partner(f, d, n_fs, 1)}, device_id_type=MESH)
    for d in range(1, n_tp):
        pl.semaphore_signal(barrier, inc=1, device_id={"tp": lax.rem(t + d, n_tp)}, device_id_type=MESH)
    pl.semaphore_signal(barrier, inc=1, device_id={"sp": nxt}, device_id_type=MESH)
    pl.semaphore_signal(barrier, inc=1, device_id={"sp": prv}, device_id_type=MESH)
    pl.semaphore_wait(barrier, n_fs - 1 + n_tp - 1 + 2)

    my_half = pl.ds(pl.multiple_of(t * half, half), half)
    tok_copies = []
    for d in range(1, n_fs):
        c = pltpu.make_async_remote_copy(
            tok.at[my_half], tok_all.at[d - 1, my_half], tok_s.at[d - 1], tok_r.at[d - 1],
            device_id={"fs": partner(f, d, n_fs, 1)}, device_id_type=MESH,
        )
        c.start()
        tok_copies.append(c)
    for c in ocopies:
        c.start()

    for c in wcopies:
        c.wait()
    step = 256
    order = (1, 2, 0, 3, 4, 5)

    @pl.loop(0, width // step)
    def _(i):
        sl = pl.ds(pl.multiple_of(i * step, step), step)
        for j in range(3):
            wcat[sl, j * 2 * DK:(j + 1) * 2 * DK] = jnp.concatenate(
                [wv[order[2 * j], sl, :], wv[order[2 * j + 1], sl, :]], axis=1
            )

    blk = 32

    def project(src_ref):
        @pl.loop(0, rows // blk)
        def _(i):
            sl = pl.ds(pl.multiple_of(i * blk, blk), blk)
            x = src_ref[sl, :].astype(jnp.float32)
            ms = jnp.mean(x * x, axis=-1, keepdims=True)
            nrm[sl, :] = (x * lax.rsqrt(ms + EPS) * gain[...]).astype(jnp.bfloat16)

        return dot_nn(nrm[...], wcat[...]).astype(jnp.bfloat16)

    own = project(tok)
    kvall[z, f] = own[:, : 2 * DK]
    pr[f, 0] = own[:, 2 * DK: 4 * DK]
    pr[f, 1] = own[:, 4 * DK:]

    relays = {}
    for d in range(1, n_fs):
        tok_copies[d - 1].wait_recv()
        for e in range(1, n_tp):
            c = pltpu.make_async_remote_copy(
                tok_all.at[d - 1, my_half], tok_all.at[d - 1, my_half],
                rel_s.at[d - 1, e - 1], rel_r.at[d - 1, e - 1],
                device_id={"tp": lax.rem(t + e, n_tp)}, device_id_type=MESH,
            )
            c.start()
            relays[d, e] = c
        for e in range(1, n_tp):
            relays[d, e].wait_recv()
        got = project(tok_all.at[d - 1])
        to = partner(f, d, n_fs, -1)
        psend[d - 1] = got[:, : 2 * DK]
        osend[d - 1, 0] = got[:, 2 * DK: 4 * DK]
        osend[d - 1, 1] = got[:, 4 * DK:]
        ca = pltpu.make_async_remote_copy(
            psend.at[d - 1], kvall.at[z, f], a_s.at[d - 1], a_r.at[d - 1],
            device_id={"fs": to}, device_id_type=MESH,
        )
        ca.start()
        cb = pltpu.make_async_remote_copy(
            osend.at[d - 1], pr.at[f], b_s.at[d - 1], b_r.at[d - 1],
            device_id={"fs": to}, device_id_type=MESH,
        )
        cb.start()
        relays[d, "a"] = ca
        relays[d, "b"] = cb

    def forward(c, p):
        return pltpu.make_async_remote_copy(
            kvall.at[c, p], kvall.at[c, p], kv_s.at[c, p], kv_r.at[c, p],
            device_id={"sp": nxt}, device_id_type=MESH,
        )

    has_next = z + 1 < n_sp
    for d in range(n_fs):
        if d:
            relays[d, "a"].wait_recv()
        p = partner(f, d, n_fs, 1)

        @pl.when(has_next)
        def _():
            forward(z, p).start()

    for d in range(1, n_fs):
        relays[d, "b"].wait_recv()

    ri_row = lax.broadcasted_iota(jnp.int32, (rows, DV), 0)
    sub_pos = lax.rem(ri_row, SUB)
    tri = (
        lax.broadcasted_iota(jnp.int32, (rows, rows), 0)
        >= lax.broadcasted_iota(jnp.int32, (rows, rows), 1)
    )
    trif = tri.astype(jnp.float32)
    sc = scale[...]
    tails = []
    gates = []
    for h in range(heads):
        rf = jnp.concatenate([pr[2 * h, 1, :, :DK], pr[2 * h + 1, 1, :, :DK]], axis=1).astype(jnp.float32)
        ri = jnp.concatenate([pr[2 * h, 1, :, DK:], pr[2 * h + 1, 1, :, DK:]], axis=1).astype(jnp.float32)
        lb = lower[h: h + 1, :]
        g = sc * jnp.log(lb + (1.0 - lb) * jax.nn.sigmoid(rf))
        kk = 1.0 - jnp.exp(g)
        a = jnp.dot(trif, g, preferred_element_type=jnp.float32, precision=lax.Precision.HIGHEST)
        last = a[rows - 1: rows, :]
        kd = (kk * jnp.exp(last - a)).astype(jnp.bfloat16)
        s_out[h] = dot_nn(ri.T.astype(jnp.bfloat16), kd)
        tails.append(jnp.exp(last))
        gates.append((a, kk, ri))

    def send_state():
        return pltpu.make_async_remote_copy(
            send_st, s_in, st_s, st_r, device_id={"sp": nxt}, device_id_type=MESH
        )

    @pl.when((z == 0) & has_next)
    def _():
        send_st[...] = s_out[...].astype(st_dtype)
        send_state().start()

    def attend(c, first):
        for h in range(heads):
            vh = jnp.concatenate([kvall[c, 2 * h, :, DK:], kvall[c, 2 * h + 1, :, DK:]], axis=1)
            for m in range(2):
                i = 2 * h + m
                sco = dot_nt(pr[i, 0, :, :DK], kvall[c, i, :, :DK]) * DK ** (-0.5)
                if first:
                    sco = jnp.where(tri, sco, NEG)
                    top = jnp.max(sco, axis=-1, keepdims=True)
                    e = jnp.exp(sco - top)
                    l_s[i] = jnp.sum(e, axis=-1, keepdims=True)
                    acc[i] = dot_nn(e.astype(jnp.bfloat16), vh)
                    m_s[i] = top
                else:
                    old = m_s[i]
                    top = jnp.maximum(old, jnp.max(sco, axis=-1, keepdims=True))
                    e = jnp.exp(sco - top)
                    shrink = jnp.exp(old - top)
                    l_s[i] = l_s[i] * shrink + jnp.sum(e, axis=-1, keepdims=True)
                    acc[i] = acc[i] * shrink + dot_nn(e.astype(jnp.bfloat16), vh)
                    m_s[i] = top

    attend(z, True)

    for h in range(heads):
        a, kk, ri = gates[h]
        rq = jnp.concatenate([pr[2 * h, 0, :, DK:], pr[2 * h + 1, 0, :, DK:]], axis=1).astype(jnp.float32)
        qdec[h] = (rq * jnp.exp(a)).astype(jnp.bfloat16)
        smat[h, 0:SUB, :] = jnp.zeros((SUB, rows), jnp.bfloat16)
        for i in range(1, rows // SUB):
            lo = i * SUB
            ref = a[lo - 1: lo, :]
            qd = (rq[lo: lo + SUB] * jnp.exp(a[lo: lo + SUB] - ref)).astype(jnp.bfloat16)
            kd = (kk * jnp.exp(jnp.where(ri_row < lo, ref - a, NEG))).astype(jnp.bfloat16)
            smat[h, lo: lo + SUB, :] = dot_nt(qd, kd).astype(jnp.bfloat16)
        o = dot_nn(smat[h], ri.astype(jnp.bfloat16))
        o = o + jnp.sum(rq * kk, axis=-1, keepdims=True) * ri
        for d in range(1, SUB):
            valid = sub_pos >= d
            dec = jnp.exp(jnp.where(valid, a - pltpu.roll(a, d, 0), NEG))
            col = jnp.sum(rq * dec * pltpu.roll(kk, d, 0), axis=-1, keepdims=True)
            o = o + col * pltpu.roll(ri, d, 0)
        olocal[h] = o

    @pl.loop(0, z)
    def _(s):
        c = z - 1 - s
        for p in range(n_fs):
            cp = forward(c, p)
            cp.wait_recv()

            @pl.when(has_next)
            def _():
                cp.start()

        attend(c, False)

    @pl.when(z > 0)
    def _():
        send_state().wait_recv()

    @pl.when((z > 0) & has_next)
    def _():
        for h in range(heads):
            send_st[h] = (tails[h] * s_in[h].astype(jnp.float32) + s_out[h]).astype(st_dtype)
        send_state().start()

    @pl.when(z > 0)
    def _():
        for h in range(heads):
            olocal[h] = olocal[h] + dot_nt(qdec[h], s_in[h].astype(jnp.bfloat16))

    atts, recs = [], []
    ag, rg = att_gain[...], rec_gain[...]
    lane = lax.broadcasted_iota(jnp.int32, (rows, DV), 1)
    lses = jnp.zeros((rows, DV), jnp.float32)
    for h in range(heads):
        x = acc[2 * h] / l_s[2 * h] - lam[0, h] * (acc[2 * h + 1] / l_s[2 * h + 1])
        ms = jnp.mean(x * x, axis=-1, keepdims=True)
        atts.append((x * lax.rsqrt(ms + EPS) * ag * 0.8).astype(jnp.bfloat16))
        o = olocal[h]
        ms = jnp.mean(o * o, axis=-1, keepdims=True)
        recs.append((o * lax.rsqrt(ms + EPS) * rg).astype(jnp.bfloat16))
        lses = jnp.where(lane == h, m_s[2 * h] + jnp.log(l_s[2 * h]), lses)
    lse[...] = lses.T[:heads, :]
    att = jnp.concatenate(atts, axis=1)
    rec = jnp.concatenate(recs, axis=1)
    for c in ocopies:
        c.wait()
    pieces = part.shape[0]
    cols = part.shape[2]
    swaps = []
    for j in range(pieces):
        sl = slice(j * cols, (j + 1) * cols)
        part[j] = (dot_nn(att, aov[:, sl]) + dot_nn(rec, rov[:, sl])).astype(jnp.bfloat16)
        for e in range(1, n_tp):
            c = pltpu.make_async_remote_copy(
                part.at[j], oprecv.at[e - 1, j], op_s.at[e - 1, j], op_r.at[e - 1, j],
                device_id={"tp": lax.rem(t + e, n_tp)}, device_id_type=MESH,
            )
            c.start()
            swaps.append((j, e, c))
    for j in range(pieces):
        total = part[j].astype(jnp.float32)
        for jj, e, c in swaps:
            if jj == j:
                c.wait_recv()
                total = total + oprecv[e - 1, j].astype(jnp.float32)
        mixed[:, j * cols:(j + 1) * cols] = total.astype(jnp.bfloat16)

    for c in tok_copies:
        c.wait_send()
    for d in range(1, n_fs):
        for e in range(1, n_tp):
            relays[d, e].wait_send()
        relays[d, "a"].wait_send()
        relays[d, "b"].wait_send()
    for _, _, c in swaps:
        c.wait_send()

    @pl.when(has_next)
    def _():
        send_state().wait_send()

        @pl.loop(0, z + 1)
        def _(c):
            for p in range(n_fs):
                forward(c, p).wait_send()


def solution(mesh):
    n_sp, n_fs, n_tp = (mesh.shape[k] for k in ("sp", "fs", "tp"))
    st_dtype = jnp.bfloat16 if n_sp <= 8 else jnp.float32

    def on_device(
        tokens, in_gain, wq, wk, wvv, wrq, wrf, wri, lam, lower, scale, att_gain, rec_gain, aow, row_w
    ):
        rows, width = tokens.shape
        heads = lower.shape[0]
        assert heads * 2 == n_fs and rows % (8 * n_tp) == 0
        vm = pl.BlockSpec(memory_space=pltpu.VMEM)
        sm = pl.BlockSpec(memory_space=pltpu.SMEM)
        hbm = pl.BlockSpec(memory_space=pl.ANY)
        bf, f32 = jnp.bfloat16, jnp.float32
        dma = pltpu.SemaphoreType.DMA
        peers = n_fs - 1
        pieces = 4
        return pl.pallas_call(
            functools.partial(kernel, n_sp, n_fs, n_tp, st_dtype),
            out_shape=(
                jax.ShapeDtypeStruct((rows, width), bf),
                jax.ShapeDtypeStruct((heads, rows), f32),
            ),
            in_specs=[vm, vm] + [hbm] * 6 + [sm, vm, vm, vm, vm, hbm, hbm],
            out_specs=(vm, vm),
            scratch_shapes=[
                pltpu.VMEM((6, width, wq.shape[1]), bf),
                pltpu.VMEM(aow.shape, bf),
                pltpu.VMEM(row_w.shape, bf),
                pltpu.VMEM((width, 6 * DK), bf),
                pltpu.VMEM((peers, rows, width), bf),
                pltpu.VMEM((rows, width), bf),
                pltpu.VMEM((peers, rows, 2 * DK), bf),
                pltpu.VMEM((peers, 2, rows, 2 * DK), bf),
                pltpu.VMEM((n_sp, n_fs, rows, 2 * DK), bf),
                pltpu.VMEM((n_fs, 2, rows, 2 * DK), bf),
                pltpu.VMEM((n_tp - 1, pieces, rows, width // pieces), bf),
                pltpu.VMEM((pieces, rows, width // pieces), bf),
                pltpu.VMEM((heads, rows, rows), bf),
                pltpu.VMEM((heads, rows, DV), f32),
                pltpu.VMEM((heads, rows, DV), bf),
                pltpu.VMEM((heads, DV, DV), st_dtype),
                pltpu.VMEM((heads, DV, DV), st_dtype),
                pltpu.VMEM((heads, DV, DV), f32),
                pltpu.VMEM((2 * heads, rows, 1), f32),
                pltpu.VMEM((2 * heads, rows, 1), f32),
                pltpu.VMEM((2 * heads, rows, DV), f32),
                dma((6,)), dma((2,)),
                dma((peers,)), dma((peers,)),
                dma((peers, n_tp - 1)), dma((peers, n_tp - 1)),
                dma((peers,)), dma((peers,)), dma((peers,)), dma((peers,)),
                dma((n_sp, n_fs)), dma((n_sp, n_fs)),
                dma, dma,
                dma((n_tp - 1, pieces)), dma((n_tp - 1, pieces)),
            ],
            compiler_params=pltpu.CompilerParams(
                collective_id=0, has_side_effects=True, vmem_limit_bytes=60 * 1024 * 1024
            ),
            name="mixer",
        )(
            tokens, in_gain[None], wq, wk, wvv, wrq, wrf, wri, lam[None], lower, scale[:, None],
            att_gain[None], rec_gain[None], aow, row_w,
        )

    col = P(None, ("tp", "fs"))
    return jax.shard_map(
        on_device,
        mesh=mesh,
        in_specs=(
            P(("fs", "sp"), None), P(), col, col, col, col, col, col,
            P("tp"), P("tp", None), P(("fs", "sp")), P(), P(), P("tp", None), P("tp", None),
        ),
        out_specs=(P(("fs", "sp"), None), P("tp", ("fs", "sp"))),
        check_vma=False,
    )
```

```python
import functools

import jax
import jax.numpy as jnp
from jax import lax
from jax.experimental import pallas as pl
from jax.experimental.pallas import tpu as pltpu
from jax.sharding import PartitionSpec as P

DK = 64
DV = 128
SUB = 16
GROUPS = 2
EPS = 1e-06
NEG = -1e30
MESH = pl.DeviceIdType.MESH


def dot_nt(a, b):
    return lax.dot_general(a, b, (((1,), (1,)), ((), ())), preferred_element_type=jnp.float32)


def dot_nn(a, b):
    return jnp.dot(a, b, preferred_element_type=jnp.float32)


def partner(f, d, n, sign):
    if n & (n - 1):
        return lax.rem(f + sign * d + n, n)
    out, bit = 0, 1
    while bit < n:
        mine = lax.rem(f // bit, 2)
        out = out + bit * ((1 - mine) if d & bit else mine)
        bit *= 2
    return out


def kernel(
    n_sp, n_fs, n_tp, st_dtype,
    tok, gain, w0, w1, w2, w3, w4, w5, lam, lower, scale, att_gain, rec_gain, aow, row_w,
    parts, lse,
    aov, rov, wcat, tok_all, nrm, psend, osend, kvall, pr,
    smat, olocal, qdec, gate, send_st, s_in, s_out, m_s, l_s, acc,
    w_sem, o_sem, tok_s, tok_r, rel_s, rel_r, a_s, a_r, b_s, b_r, kv_s, kv_r, st_s, st_r, op_s, op_r,
):
    z, f, t = lax.axis_index("sp"), lax.axis_index("fs"), lax.axis_index("tp")
    rows, width = tok.shape
    heads = n_fs // 2
    grp = rows // GROUPS
    mine = grp // n_tp
    sub = mine // 2
    nxt, prv = lax.rem(z + 1, n_sp), lax.rem(z + n_sp - 1, n_sp)
    has_next = z + 1 < n_sp
    hop = n_fs == 4

    order = (2, 0, 1, 3, 4, 5)
    wcopies = [
        pltpu.make_async_copy(w, wcat.at[pl.ds(order[i] * DK, DK)], w_sem.at[i])
        for i, w in enumerate((w0, w1, w2, w3, w4, w5))
    ]
    for c in wcopies:
        c.start()
    ocopies = [
        pltpu.make_async_copy(aow, aov, o_sem.at[0]),
        pltpu.make_async_copy(row_w, rov, o_sem.at[1]),
    ]

    barrier = pltpu.get_barrier_semaphore()
    for d in range(1, n_fs):
        pl.semaphore_signal(barrier, inc=1, device_id={"fs": partner(f, d, n_fs, 1)}, device_id_type=MESH)
    for d in range(1, n_tp):
        pl.semaphore_signal(barrier, inc=1, device_id={"tp": lax.rem(t + d, n_tp)}, device_id_type=MESH)
    pl.semaphore_signal(barrier, inc=1, device_id={"sp": nxt}, device_id_type=MESH)
    pl.semaphore_signal(barrier, inc=1, device_id={"sp": prv}, device_id_type=MESH)
    pl.semaphore_wait(barrier, n_fs - 1 + n_tp - 1 + 2)

    def span(g, u):
        return pl.ds(pl.multiple_of(g * grp + t * mine + u * sub, sub), sub)

    def token_copy(g, d, u):
        if hop and d == 3:
            src, to = (tok_all.at[0], 2) if u == 0 else (tok_all.at[1], 1)
        else:
            src, to = tok, d
        return pltpu.make_async_remote_copy(
            src.at[span(g, u)], tok_all.at[d - 1, span(g, u)],
            tok_s.at[g, d - 1, u], tok_r.at[g, d - 1, u],
            device_id={"fs": partner(f, to, n_fs, 1)}, device_id_type=MESH,
        )

    def relay(g, d, u, e):
        return pltpu.make_async_remote_copy(
            tok_all.at[d - 1, span(g, u)], tok_all.at[d - 1, span(g, u)],
            rel_s.at[g, d - 1, u, e - 1], rel_r.at[g, d - 1, u, e - 1],
            device_id={"tp": lax.rem(t + e, n_tp)}, device_id_type=MESH,
        )

    def relay_wait(g, d, u, e):
        other = lax.rem(t + n_tp - e, n_tp)
        at = pl.ds(pl.multiple_of(g * grp + other * mine + u * sub, sub), sub)
        pltpu.make_async_remote_copy(
            tok_all.at[d - 1, at], tok_all.at[d - 1, at],
            rel_s.at[g, d - 1, u, e - 1], rel_r.at[g, d - 1, u, e - 1],
            device_id={"tp": lax.rem(t + e, n_tp)}, device_id_type=MESH,
        ).wait_recv()

    def direct(g):
        if hop:
            seq = [(1, 0), (2, 1), (1, 1), (2, 0)]
        else:
            seq = [(d, u) for d in range(1, n_fs) for u in range(2)]
        for d, u in seq:
            token_copy(g, d, u).start()

    def arrive(g, d, u):
        token_copy(g, d, u).wait_recv()
        if hop and (d, u) in ((1, 0), (2, 1)):
            token_copy(g, 3, u).start()
        for e in range(1, n_tp):
            relay(g, d, u, e).start()

    def first_arrivals(g):
        if hop:
            arrive(g, 1, 0)
            arrive(g, 2, 1)

    def last_arrivals(g):
        if hop:
            seq = [(1, 1), (2, 0), (3, 0), (3, 1)]
        else:
            seq = [(d, u) for d in range(1, n_fs) for u in range(2)]
        for d, u in seq:
            arrive(g, d, u)
        for d in range(1, n_fs):
            for u in range(2):
                for e in range(1, n_tp):
                    relay_wait(g, d, u, e)

    blk = min(32, grp)

    def normalise(src_ref, first, to):
        @pl.loop(0, grp // blk)
        def _(i):
            x = src_ref[pl.ds(pl.multiple_of(first + i * blk, blk), blk), :].astype(jnp.float32)
            ms = jnp.mean(x * x, axis=-1, keepdims=True)
            nrm[pl.ds(pl.multiple_of(to + i * blk, blk), blk), :] = (
                x * lax.rsqrt(ms + EPS) * gain[...]
            ).astype(jnp.bfloat16)

    def back(g, d):
        to = partner(f, d, n_fs, -1)
        return (
            pltpu.make_async_remote_copy(
                psend.at[g, d - 1], kvall.at[z, g, f], a_s.at[g, d - 1], a_r.at[g, d - 1],
                device_id={"fs": to}, device_id_type=MESH,
            ),
            pltpu.make_async_remote_copy(
                osend.at[g, d - 1], pr.at[f, g], b_s.at[g, d - 1], b_r.at[g, d - 1],
                device_id={"fs": to}, device_id_type=MESH,
            ),
        )

    def project(g):
        for d in range(1, n_fs):
            normalise(tok_all.at[d - 1], g * grp, d * grp)
        got = dot_nt(nrm[...], wcat[...]).astype(jnp.bfloat16)
        for d in range(1, n_fs):
            lo = d * grp
            psend[g, d - 1] = got[lo: lo + grp, : 2 * DK]
            osend[g, d - 1, 0] = got[lo: lo + grp, 2 * DK: 4 * DK]
            osend[g, d - 1, 1] = got[lo: lo + grp, 4 * DK:]
        kvall[z, g, f] = got[:grp, : 2 * DK]
        pr[f, g, 0] = got[:grp, 2 * DK: 4 * DK]
        pr[f, g, 1] = got[:grp, 4 * DK:]
        for d in range(1, n_fs):
            back(g, d)[0].start()
        for d in range(1, n_fs):
            back(g, d)[1].start()

    def chain(c, g):
        return pltpu.make_async_remote_copy(
            kvall.at[c, g], kvall.at[c, g], kv_s.at[c, g], kv_r.at[c, g],
            device_id={"sp": nxt}, device_id_type=MESH,
        )

    def own_chain(g):
        for d in range(1, n_fs):
            back(g, d)[0].wait_recv()

        @pl.when(has_next)
        def _():
            chain(z, g).start()

    def pass_on(c, g):
        chain(c, g).wait_recv()

        @pl.when(has_next)
        def _():
            chain(c, g).start()

    def forward(k):
        s, g = k // GROUPS, k % GROUPS
        if s < n_sp - 1:
            @pl.when(z > s)
            def _():
                pass_on(z - 1 - s, g)

    direct(0)
    for c in ocopies:
        c.start()
    normalise(tok, 0, 0)
    first_arrivals(0)
    for g in range(1, GROUPS):
        direct(g)
    for c in wcopies:
        c.wait()
    last_arrivals(0)
    project(0)
    for g in range(1, GROUPS):
        normalise(tok, g * grp, 0)
        first_arrivals(g)
        own_chain(g - 1)
        last_arrivals(g)
        project(g)
    forward(0)
    own_chain(GROUPS - 1)
    for g in range(GROUPS):
        for d in range(1, n_fs):
            back(g, d)[1].wait_recv()

    def column(i, j, part):
        return pr[i, :, j, :, part * DK:(part + 1) * DK].reshape(rows, DK)

    def wide(h, j, part):
        return jnp.concatenate([column(2 * h, j, part), column(2 * h + 1, j, part)], axis=1)

    row_at = lax.broadcasted_iota(jnp.int32, (rows, DV), 0)
    sub_pos = lax.rem(row_at, SUB)
    tri = (
        lax.broadcasted_iota(jnp.int32, (rows, rows), 0)
        >= lax.broadcasted_iota(jnp.int32, (rows, rows), 1)
    )
    trif = tri.astype(jnp.float32)
    sc = jnp.broadcast_to(scale[...], (DV, rows)).T
    tails = []
    for h in range(heads):
        rf = wide(h, 1, 0).astype(jnp.float32)
        ri = wide(h, 1, 1).astype(jnp.float32)
        lb = lower[h: h + 1, :]
        g = sc * jnp.log(lb + (1.0 - lb) * jax.nn.sigmoid(rf))
        kk = 1.0 - jnp.exp(g)
        a = jnp.dot(trif, g, preferred_element_type=jnp.float32, precision=lax.Precision.HIGHEST)
        last = a[rows - 1: rows, :]
        kd = (kk * jnp.exp(last - a)).astype(jnp.bfloat16)
        s_out[h] = dot_nn(ri.T.astype(jnp.bfloat16), kd)
        tails.append(jnp.exp(last))
        gate[h, 0] = a
        gate[h, 1] = kk

    def send_state():
        return pltpu.make_async_remote_copy(
            send_st, s_in, st_s, st_r, device_id={"sp": nxt}, device_id_type=MESH
        )

    @pl.when((z == 0) & has_next)
    def _():
        send_st[...] = s_out[...].astype(st_dtype)
        send_state().start()

    def carry(when):
        @pl.when(when)
        def _():
            send_state().wait_recv()

        @pl.when(when & has_next)
        def _():
            for h in range(heads):
                send_st[h] = (tails[h] * s_in[h].astype(jnp.float32) + s_out[h]).astype(st_dtype)
            send_state().start()

    def attend(c, first):
        for h in range(heads):
            vh = jnp.concatenate(
                [
                    kvall[c, :, 2 * h, :, DK:].reshape(rows, DK),
                    kvall[c, :, 2 * h + 1, :, DK:].reshape(rows, DK),
                ],
                axis=1,
            )
            for m in range(2):
                i = 2 * h + m
                keys = kvall[c, :, i, :, :DK].reshape(rows, DK)
                sco = dot_nt(column(i, 0, 0), keys) * DK ** (-0.5)
                if first:
                    sco = jnp.where(tri, sco, NEG)
                    top = jnp.max(sco, axis=-1, keepdims=True)
                    e = jnp.exp(sco - top)
                    l_s[i] = jnp.sum(e, axis=-1, keepdims=True)
                    acc[i] = dot_nn(e.astype(jnp.bfloat16), vh)
                    m_s[i] = top
                else:
                    old = m_s[i]
                    top = jnp.maximum(old, jnp.max(sco, axis=-1, keepdims=True))
                    e = jnp.exp(sco - top)
                    shrink = jnp.exp(old - top)
                    l_s[i] = l_s[i] * shrink + jnp.sum(e, axis=-1, keepdims=True)
                    acc[i] = acc[i] * shrink + dot_nn(e.astype(jnp.bfloat16), vh)
                    m_s[i] = top

    def recur(h):
        a, kk = gate[h, 0], gate[h, 1]
        ri = wide(h, 1, 1).astype(jnp.float32)
        rq = wide(h, 0, 1).astype(jnp.float32)
        qdec[h] = (rq * jnp.exp(a)).astype(jnp.bfloat16)
        smat[h, 0:SUB, :] = jnp.zeros((SUB, rows), jnp.bfloat16)
        for i in range(1, rows // SUB):
            lo = i * SUB
            ref = a[lo - 1: lo, :]
            qd = (rq[lo: lo + SUB] * jnp.exp(a[lo: lo + SUB] - ref)).astype(jnp.bfloat16)
            kd = (kk * jnp.exp(jnp.where(row_at < lo, ref - a, NEG))).astype(jnp.bfloat16)
            smat[h, lo: lo + SUB, :] = dot_nt(qd, kd).astype(jnp.bfloat16)
        o = dot_nn(smat[h], ri.astype(jnp.bfloat16))
        o = o + jnp.sum(rq * kk, axis=-1, keepdims=True) * ri
        for d in range(1, SUB):
            dec = jnp.exp(jnp.where(sub_pos >= d, a - pltpu.roll(a, d, 0), NEG))
            col = jnp.sum(rq * dec * pltpu.roll(kk, d, 0), axis=-1, keepdims=True)
            o = o + col * pltpu.roll(ri, d, 0)
        olocal[h] = o

    forward(1)
    carry(z == 1)
    forward(2)
    attend(z, True)
    forward(3)
    recur(0)
    carry(z == 2)
    forward(4)

    @pl.when(z > 0)
    def _():
        attend(z - 1, False)

    forward(5)
    for h in range(1, heads):
        recur(h)

    @pl.loop(1, z)
    def _(s):
        c = z - 1 - s

        @pl.when(s >= 3)
        def _():
            for g in range(GROUPS):
                pass_on(c, g)

        attend(c, False)

    carry(z > 2)

    @pl.when(z > 0)
    def _():
        for h in range(heads):
            olocal[h] = olocal[h] + dot_nt(qdec[h], s_in[h].astype(jnp.bfloat16))

    atts, recs = [], []
    ag, rg = att_gain[...], rec_gain[...]
    lane = lax.broadcasted_iota(jnp.int32, (rows, DV), 1)
    lses = jnp.zeros((rows, DV), jnp.float32)
    for h in range(heads):
        x = acc[2 * h] / l_s[2 * h] - lam[0, h] * (acc[2 * h + 1] / l_s[2 * h + 1])
        ms = jnp.mean(x * x, axis=-1, keepdims=True)
        atts.append((x * lax.rsqrt(ms + EPS) * ag * 0.8).astype(jnp.bfloat16))
        o = olocal[h]
        ms = jnp.mean(o * o, axis=-1, keepdims=True)
        recs.append((o * lax.rsqrt(ms + EPS) * rg).astype(jnp.bfloat16))
        lses = jnp.where(lane == h, m_s[2 * h] + jnp.log(l_s[2 * h]), lses)
    lse[...] = lses.T[:heads, :]
    att = jnp.concatenate(atts, axis=1)
    rec = jnp.concatenate(recs, axis=1)
    for c in ocopies:
        c.wait()
    pieces = 4
    cols = width // pieces
    swaps = []
    for j in range(pieces):
        sl = slice(j * cols, (j + 1) * cols)
        parts[0, :, sl] = (dot_nn(att, aov[:, sl]) + dot_nn(rec, rov[:, sl])).astype(jnp.bfloat16)
        for e in range(1, n_tp):
            c = pltpu.make_async_remote_copy(
                parts.at[0, :, sl], parts.at[e, :, sl], op_s.at[e - 1, j], op_r.at[e - 1, j],
                device_id={"tp": lax.rem(t + e, n_tp)}, device_id_type=MESH,
            )
            c.start()
            swaps.append(c)

    for g in range(GROUPS):
        for d in range(1, n_fs):
            for u in range(2):
                token_copy(g, d, u).wait_send()
                for e in range(1, n_tp):
                    relay(g, d, u, e).wait_send()
            for c in back(g, d):
                c.wait_send()

    @pl.when(has_next)
    def _():
        send_state().wait_send()

        @pl.loop(0, z + 1)
        def _(c):
            for g in range(GROUPS):
                chain(c, g).wait_send()

    for c in swaps:
        c.wait()


def finish(parts, lse_in, mixed, lse):
    total = parts[0].astype(jnp.float32)
    for e in range(1, parts.shape[0]):
        total = total + parts[e].astype(jnp.float32)
    mixed[...] = total.astype(jnp.bfloat16)
    lse[...] = lse_in[...]


def solution(mesh):
    n_sp, n_fs, n_tp = (mesh.shape[k] for k in ("sp", "fs", "tp"))
    st_dtype = jnp.bfloat16 if n_sp <= 8 else jnp.float32

    def on_device(
        tokens, in_gain, wq, wk, wvv, wrq, wrf, wri, lam, lower, scale, att_gain, rec_gain, aow, row_w
    ):
        rows, width = tokens.shape
        heads = lower.shape[0]
        assert heads * 2 == n_fs and rows % (8 * n_tp) == 0
        vm = pl.BlockSpec(memory_space=pltpu.VMEM)
        sm = pl.BlockSpec(memory_space=pltpu.SMEM)
        hbm = pl.BlockSpec(memory_space=pl.ANY)
        bf, f32 = jnp.bfloat16, jnp.float32
        dma = pltpu.SemaphoreType.DMA
        peers = n_fs - 1
        pieces = 4
        grp = rows // GROUPS
        parts, lse = pl.pallas_call(
            functools.partial(kernel, n_sp, n_fs, n_tp, st_dtype),
            out_shape=(
                jax.ShapeDtypeStruct((n_tp, rows, width), bf),
                jax.ShapeDtypeStruct((heads, rows), f32),
            ),
            in_specs=[vm, vm] + [hbm] * 6 + [sm, vm, vm, vm, vm, hbm, hbm],
            out_specs=(vm, vm),
            scratch_shapes=[
                pltpu.VMEM(aow.shape, bf),
                pltpu.VMEM(row_w.shape, bf),
                pltpu.VMEM((6 * DK, width), bf),
                pltpu.VMEM((peers, rows, width), bf),
                pltpu.VMEM((n_fs * grp, width), bf),
                pltpu.VMEM((GROUPS, peers, grp, 2 * DK), bf),
                pltpu.VMEM((GROUPS, peers, 2, grp, 2 * DK), bf),
                pltpu.VMEM((n_sp, GROUPS, n_fs, grp, 2 * DK), bf),
                pltpu.VMEM((n_fs, GROUPS, 2, grp, 2 * DK), bf),
                pltpu.VMEM((heads, rows, rows), bf),
                pltpu.VMEM((heads, rows, DV), f32),
                pltpu.VMEM((heads, rows, DV), bf),
                pltpu.VMEM((heads, 2, rows, DV), f32),
                pltpu.VMEM((heads, DV, DV), st_dtype),
                pltpu.VMEM((heads, DV, DV), st_dtype),
                pltpu.VMEM((heads, DV, DV), f32),
                pltpu.VMEM((2 * heads, rows, 1), f32),
                pltpu.VMEM((2 * heads, rows, 1), f32),
                pltpu.VMEM((2 * heads, rows, DV), f32),
                dma((6,)), dma((2,)),
                dma((GROUPS, peers, 2)), dma((GROUPS, peers, 2)),
                dma((GROUPS, peers, 2, n_tp - 1)), dma((GROUPS, peers, 2, n_tp - 1)),
                dma((GROUPS, peers)), dma((GROUPS, peers)), dma((GROUPS, peers)), dma((GROUPS, peers)),
                dma((n_sp, GROUPS)), dma((n_sp, GROUPS)),
                dma, dma,
                dma((n_tp - 1, pieces)), dma((n_tp - 1, pieces)),
            ],
            compiler_params=pltpu.CompilerParams(
                collective_id=0, has_side_effects=True, vmem_limit_bytes=56 * 1024 * 1024
            ),
            name="mixer",
        )(
            tokens, in_gain[None], wq.T, wk.T, wvv.T, wrq.T, wrf.T, wri.T, lam[None], lower, scale[None],
            att_gain[None], rec_gain[None], aow, row_w,
        )
        half = width // 2
        return pl.pallas_call(
            finish,
            grid=(2,),
            out_shape=(
                jax.ShapeDtypeStruct((rows, width), bf),
                jax.ShapeDtypeStruct((heads, rows), f32),
            ),
            in_specs=[
                pl.BlockSpec((n_tp, rows, half), lambda i: (0, 0, i)),
                pl.BlockSpec((heads, rows), lambda i: (0, 0)),
            ],
            out_specs=(
                pl.BlockSpec((rows, half), lambda i: (0, i)),
                pl.BlockSpec((heads, rows), lambda i: (0, 0)),
            ),
            name="finish",
        )(parts, lse)

    col = P(None, ("tp", "fs"))
    return jax.shard_map(
        on_device,
        mesh=mesh,
        in_specs=(
            P(("fs", "sp"), None), P(), col, col, col, col, col, col,
            P("tp"), P("tp", None), P(("fs", "sp")), P(), P(), P("tp", None), P("tp", None),
        ),
        out_specs=(P(("fs", "sp"), None), P("tp", ("fs", "sp"))),
        check_vma=False,
    )
```

```python
import functools

import jax
import jax.numpy as jnp
from jax import lax
from jax.experimental import pallas as pl
from jax.experimental.pallas import tpu as pltpu
from jax.sharding import PartitionSpec as P

DK = 64
DV = 128
SUB = 16
EPS = 1e-06
NEG = -1e30
MESH = pl.DeviceIdType.MESH


def dot_nt(a, b):
    return lax.dot_general(a, b, (((1,), (1,)), ((), ())), preferred_element_type=jnp.float32)


def dot_nn(a, b):
    return jnp.dot(a, b, preferred_element_type=jnp.float32)


def partner(f, d, n, sign):
    if n & (n - 1):
        return lax.rem(f + sign * d + n, n)
    out, bit = 0, 1
    while bit < n:
        mine = lax.rem(f // bit, 2)
        out = out + bit * ((1 - mine) if d & bit else mine)
        bit *= 2
    return out


def kernel(
    n_sp, n_fs, n_tp, st_dtype,
    tok, gain, w0, w1, w2, w3, w4, w5, lam, lower, scale, att_gain, rec_gain, aow, row_w,
    parts, lse,
    aov, rov, wcat, tok_all, nrm, psend, osend, kvall, pr,
    smat, olocal, qdec, send_st, s_in, s_out, m_s, l_s, acc,
    w_sem, o_sem, tok_s, tok_r, rel_s, rel_r, a_s, a_r, b_s, b_r, kv_s, kv_r, st_s, st_r, op_s, op_r,
):
    z, f, t = lax.axis_index("sp"), lax.axis_index("fs"), lax.axis_index("tp")
    rows, width = tok.shape
    half = rows // n_tp
    heads = n_fs // 2
    nxt, prv = lax.rem(z + 1, n_sp), lax.rem(z + n_sp - 1, n_sp)

    order = (2, 0, 1, 3, 4, 5)
    wcopies = [
        pltpu.make_async_copy(w, wcat.at[pl.ds(order[i] * DK, DK)], w_sem.at[i])
        for i, w in enumerate((w0, w1, w2, w3, w4, w5))
    ]
    for c in wcopies:
        c.start()
    ocopies = [
        pltpu.make_async_copy(aow, aov, o_sem.at[0]),
        pltpu.make_async_copy(row_w, rov, o_sem.at[1]),
    ]

    barrier = pltpu.get_barrier_semaphore()
    for d in range(1, n_fs):
        pl.semaphore_signal(barrier, inc=1, device_id={"fs": partner(f, d, n_fs, 1)}, device_id_type=MESH)
    for d in range(1, n_tp):
        pl.semaphore_signal(barrier, inc=1, device_id={"tp": lax.rem(t + d, n_tp)}, device_id_type=MESH)
    pl.semaphore_signal(barrier, inc=1, device_id={"sp": nxt}, device_id_type=MESH)
    pl.semaphore_signal(barrier, inc=1, device_id={"sp": prv}, device_id_type=MESH)
    pl.semaphore_wait(barrier, n_fs - 1 + n_tp - 1 + 2)

    my_half = pl.ds(pl.multiple_of(t * half, half), half)
    tok_copies = []
    for d in range(1, n_fs):
        c = pltpu.make_async_remote_copy(
            tok.at[my_half], tok_all.at[d - 1, my_half], tok_s.at[d - 1], tok_r.at[d - 1],
            device_id={"fs": partner(f, d, n_fs, 1)}, device_id_type=MESH,
        )
        c.start()
        tok_copies.append(c)
    for c in ocopies:
        c.start()

    for c in wcopies:
        c.wait()

    blk = 32

    def project(src_ref):
        @pl.loop(0, rows // blk)
        def _(i):
            sl = pl.ds(pl.multiple_of(i * blk, blk), blk)
            x = src_ref[sl, :].astype(jnp.float32)
            ms = jnp.mean(x * x, axis=-1, keepdims=True)
            nrm[sl, :] = (x * lax.rsqrt(ms + EPS) * gain[...]).astype(jnp.bfloat16)

        return dot_nt(nrm[...], wcat[...]).astype(jnp.bfloat16)

    own = project(tok)
    kvall[z, f] = own[:, : 2 * DK]
    pr[f, 0] = own[:, 2 * DK: 4 * DK]
    pr[f, 1] = own[:, 4 * DK:]

    relays = {}
    for d in range(1, n_fs):
        tok_copies[d - 1].wait_recv()
        for e in range(1, n_tp):
            c = pltpu.make_async_remote_copy(
                tok_all.at[d - 1, my_half], tok_all.at[d - 1, my_half],
                rel_s.at[d - 1, e - 1], rel_r.at[d - 1, e - 1],
                device_id={"tp": lax.rem(t + e, n_tp)}, device_id_type=MESH,
            )
            c.start()
            relays[d, e] = c
        for e in range(1, n_tp):
            relays[d, e].wait_recv()
        got = project(tok_all.at[d - 1])
        to = partner(f, d, n_fs, -1)
        psend[d - 1] = got[:, : 2 * DK]
        osend[d - 1, 0] = got[:, 2 * DK: 4 * DK]
        osend[d - 1, 1] = got[:, 4 * DK:]
        ca = pltpu.make_async_remote_copy(
            psend.at[d - 1], kvall.at[z, f], a_s.at[d - 1], a_r.at[d - 1],
            device_id={"fs": to}, device_id_type=MESH,
        )
        ca.start()
        cb = pltpu.make_async_remote_copy(
            osend.at[d - 1], pr.at[f], b_s.at[d - 1], b_r.at[d - 1],
            device_id={"fs": to}, device_id_type=MESH,
        )
        cb.start()
        relays[d, "a"] = ca
        relays[d, "b"] = cb

    def forward(c, p):
        return pltpu.make_async_remote_copy(
            kvall.at[c, p], kvall.at[c, p], kv_s.at[c, p], kv_r.at[c, p],
            device_id={"sp": nxt}, device_id_type=MESH,
        )

    has_next = z + 1 < n_sp
    for d in range(n_fs):
        if d:
            relays[d, "a"].wait_recv()
        p = partner(f, d, n_fs, 1)

        @pl.when(has_next)
        def _():
            forward(z, p).start()

    for d in range(1, n_fs):
        relays[d, "b"].wait_recv()

    ri_row = lax.broadcasted_iota(jnp.int32, (rows, DV), 0)
    sub_pos = lax.rem(ri_row, SUB)
    tri = (
        lax.broadcasted_iota(jnp.int32, (rows, rows), 0)
        >= lax.broadcasted_iota(jnp.int32, (rows, rows), 1)
    )
    trif = tri.astype(jnp.float32)
    sc = jnp.broadcast_to(scale[...], (DV, rows)).T
    tails = []
    gates = []
    for h in range(heads):
        rf = jnp.concatenate([pr[2 * h, 1, :, :DK], pr[2 * h + 1, 1, :, :DK]], axis=1).astype(jnp.float32)
        ri = jnp.concatenate([pr[2 * h, 1, :, DK:], pr[2 * h + 1, 1, :, DK:]], axis=1).astype(jnp.float32)
        lb = lower[h: h + 1, :]
        g = sc * jnp.log(lb + (1.0 - lb) * jax.nn.sigmoid(rf))
        kk = 1.0 - jnp.exp(g)
        a = jnp.dot(trif, g, preferred_element_type=jnp.float32, precision=lax.Precision.HIGHEST)
        last = a[rows - 1: rows, :]
        kd = (kk * jnp.exp(last - a)).astype(jnp.bfloat16)
        s_out[h] = dot_nn(ri.T.astype(jnp.bfloat16), kd)
        tails.append(jnp.exp(last))
        gates.append((a, kk, ri))

    def send_state():
        return pltpu.make_async_remote_copy(
            send_st, s_in, st_s, st_r, device_id={"sp": nxt}, device_id_type=MESH
        )

    @pl.when((z == 0) & has_next)
    def _():
        send_st[...] = s_out[...].astype(st_dtype)
        send_state().start()

    def attend(c, first):
        for h in range(heads):
            vh = jnp.concatenate([kvall[c, 2 * h, :, DK:], kvall[c, 2 * h + 1, :, DK:]], axis=1)
            for m in range(2):
                i = 2 * h + m
                sco = dot_nt(pr[i, 0, :, :DK], kvall[c, i, :, :DK]) * DK ** (-0.5)
                if first:
                    sco = jnp.where(tri, sco, NEG)
                    top = jnp.max(sco, axis=-1, keepdims=True)
                    e = jnp.exp(sco - top)
                    l_s[i] = jnp.sum(e, axis=-1, keepdims=True)
                    acc[i] = dot_nn(e.astype(jnp.bfloat16), vh)
                    m_s[i] = top
                else:
                    old = m_s[i]
                    top = jnp.maximum(old, jnp.max(sco, axis=-1, keepdims=True))
                    e = jnp.exp(sco - top)
                    shrink = jnp.exp(old - top)
                    l_s[i] = l_s[i] * shrink + jnp.sum(e, axis=-1, keepdims=True)
                    acc[i] = acc[i] * shrink + dot_nn(e.astype(jnp.bfloat16), vh)
                    m_s[i] = top

    attend(z, True)

    for h in range(heads):
        a, kk, ri = gates[h]
        rq = jnp.concatenate([pr[2 * h, 0, :, DK:], pr[2 * h + 1, 0, :, DK:]], axis=1).astype(jnp.float32)
        qdec[h] = (rq * jnp.exp(a)).astype(jnp.bfloat16)
        smat[h, 0:SUB, :] = jnp.zeros((SUB, rows), jnp.bfloat16)
        for i in range(1, rows // SUB):
            lo = i * SUB
            ref = a[lo - 1: lo, :]
            qd = (rq[lo: lo + SUB] * jnp.exp(a[lo: lo + SUB] - ref)).astype(jnp.bfloat16)
            kd = (kk * jnp.exp(jnp.where(ri_row < lo, ref - a, NEG))).astype(jnp.bfloat16)
            smat[h, lo: lo + SUB, :] = dot_nt(qd, kd).astype(jnp.bfloat16)
        o = dot_nn(smat[h], ri.astype(jnp.bfloat16))
        o = o + jnp.sum(rq * kk, axis=-1, keepdims=True) * ri
        for d in range(1, SUB):
            valid = sub_pos >= d
            dec = jnp.exp(jnp.where(valid, a - pltpu.roll(a, d, 0), NEG))
            col = jnp.sum(rq * dec * pltpu.roll(kk, d, 0), axis=-1, keepdims=True)
            o = o + col * pltpu.roll(ri, d, 0)
        olocal[h] = o

    @pl.loop(0, z)
    def _(s):
        c = z - 1 - s
        for p in range(n_fs):
            cp = forward(c, p)
            cp.wait_recv()

            @pl.when(has_next)
            def _():
                cp.start()

        attend(c, False)

    @pl.when(z > 0)
    def _():
        send_state().wait_recv()

    @pl.when((z > 0) & has_next)
    def _():
        for h in range(heads):
            send_st[h] = (tails[h] * s_in[h].astype(jnp.float32) + s_out[h]).astype(st_dtype)
        send_state().start()

    @pl.when(z > 0)
    def _():
        for h in range(heads):
            olocal[h] = olocal[h] + dot_nt(qdec[h], s_in[h].astype(jnp.bfloat16))

    atts, recs = [], []
    ag, rg = att_gain[...], rec_gain[...]
    lane = lax.broadcasted_iota(jnp.int32, (rows, DV), 1)
    lses = jnp.zeros((rows, DV), jnp.float32)
    for h in range(heads):
        x = acc[2 * h] / l_s[2 * h] - lam[0, h] * (acc[2 * h + 1] / l_s[2 * h + 1])
        ms = jnp.mean(x * x, axis=-1, keepdims=True)
        atts.append((x * lax.rsqrt(ms + EPS) * ag * 0.8).astype(jnp.bfloat16))
        o = olocal[h]
        ms = jnp.mean(o * o, axis=-1, keepdims=True)
        recs.append((o * lax.rsqrt(ms + EPS) * rg).astype(jnp.bfloat16))
        lses = jnp.where(lane == h, m_s[2 * h] + jnp.log(l_s[2 * h]), lses)
    lse[...] = lses.T[:heads, :]
    att = jnp.concatenate(atts, axis=1)
    rec = jnp.concatenate(recs, axis=1)
    for c in ocopies:
        c.wait()
    pieces = 4
    cols = width // pieces
    swaps = []
    for j in range(pieces):
        sl = slice(j * cols, (j + 1) * cols)
        parts[0, :, sl] = (dot_nn(att, aov[:, sl]) + dot_nn(rec, rov[:, sl])).astype(jnp.bfloat16)
        for e in range(1, n_tp):
            c = pltpu.make_async_remote_copy(
                parts.at[0, :, sl], parts.at[e, :, sl], op_s.at[e - 1, j], op_r.at[e - 1, j],
                device_id={"tp": lax.rem(t + e, n_tp)}, device_id_type=MESH,
            )
            c.start()
            swaps.append(c)

    for c in tok_copies:
        c.wait_send()
    for d in range(1, n_fs):
        for e in range(1, n_tp):
            relays[d, e].wait_send()
        relays[d, "a"].wait_send()
        relays[d, "b"].wait_send()
    @pl.when(has_next)
    def _():
        send_state().wait_send()

        @pl.loop(0, z + 1)
        def _(c):
            for p in range(n_fs):
                forward(c, p).wait_send()

    for c in swaps:
        c.wait()


def finish(parts, lse_in, mixed, lse):
    total = parts[0].astype(jnp.float32)
    for e in range(1, parts.shape[0]):
        total = total + parts[e].astype(jnp.float32)
    mixed[...] = total.astype(jnp.bfloat16)
    lse[...] = lse_in[...]


def solution(mesh):
    n_sp, n_fs, n_tp = (mesh.shape[k] for k in ("sp", "fs", "tp"))
    st_dtype = jnp.bfloat16 if n_sp <= 8 else jnp.float32

    def on_device(
        tokens, in_gain, wq, wk, wvv, wrq, wrf, wri, lam, lower, scale, att_gain, rec_gain, aow, row_w
    ):
        rows, width = tokens.shape
        heads = lower.shape[0]
        assert heads * 2 == n_fs and rows % (8 * n_tp) == 0
        vm = pl.BlockSpec(memory_space=pltpu.VMEM)
        sm = pl.BlockSpec(memory_space=pltpu.SMEM)
        hbm = pl.BlockSpec(memory_space=pl.ANY)
        bf, f32 = jnp.bfloat16, jnp.float32
        dma = pltpu.SemaphoreType.DMA
        peers = n_fs - 1
        pieces = 4
        parts, lse = pl.pallas_call(
            functools.partial(kernel, n_sp, n_fs, n_tp, st_dtype),
            out_shape=(
                jax.ShapeDtypeStruct((n_tp, rows, width), bf),
                jax.ShapeDtypeStruct((heads, rows), f32),
            ),
            in_specs=[vm, vm] + [hbm] * 6 + [sm, vm, vm, vm, vm, hbm, hbm],
            out_specs=(vm, vm),
            scratch_shapes=[
                pltpu.VMEM(aow.shape, bf),
                pltpu.VMEM(row_w.shape, bf),
                pltpu.VMEM((6 * DK, width), bf),
                pltpu.VMEM((peers, rows, width), bf),
                pltpu.VMEM((rows, width), bf),
                pltpu.VMEM((peers, rows, 2 * DK), bf),
                pltpu.VMEM((peers, 2, rows, 2 * DK), bf),
                pltpu.VMEM((n_sp, n_fs, rows, 2 * DK), bf),
                pltpu.VMEM((n_fs, 2, rows, 2 * DK), bf),
                pltpu.VMEM((heads, rows, rows), bf),
                pltpu.VMEM((heads, rows, DV), f32),
                pltpu.VMEM((heads, rows, DV), bf),
                pltpu.VMEM((heads, DV, DV), st_dtype),
                pltpu.VMEM((heads, DV, DV), st_dtype),
                pltpu.VMEM((heads, DV, DV), f32),
                pltpu.VMEM((2 * heads, rows, 1), f32),
                pltpu.VMEM((2 * heads, rows, 1), f32),
                pltpu.VMEM((2 * heads, rows, DV), f32),
                dma((6,)), dma((2,)),
                dma((peers,)), dma((peers,)),
                dma((peers, n_tp - 1)), dma((peers, n_tp - 1)),
                dma((peers,)), dma((peers,)), dma((peers,)), dma((peers,)),
                dma((n_sp, n_fs)), dma((n_sp, n_fs)),
                dma, dma,
                dma((n_tp - 1, pieces)), dma((n_tp - 1, pieces)),
            ],
            compiler_params=pltpu.CompilerParams(
                collective_id=0, has_side_effects=True, vmem_limit_bytes=56 * 1024 * 1024
            ),
            name="mixer",
        )(
            tokens, in_gain[None], wq.T, wk.T, wvv.T, wrq.T, wrf.T, wri.T, lam[None], lower, scale[None],
            att_gain[None], rec_gain[None], aow, row_w,
        )
        half = width // 2
        return pl.pallas_call(
            finish,
            grid=(2,),
            out_shape=(
                jax.ShapeDtypeStruct((rows, width), bf),
                jax.ShapeDtypeStruct((heads, rows), f32),
            ),
            in_specs=[
                pl.BlockSpec((n_tp, rows, half), lambda i: (0, 0, i)),
                pl.BlockSpec((heads, rows), lambda i: (0, 0)),
            ],
            out_specs=(
                pl.BlockSpec((rows, half), lambda i: (0, i)),
                pl.BlockSpec((heads, rows), lambda i: (0, 0)),
            ),
            name="finish",
        )(parts, lse)

    col = P(None, ("tp", "fs"))
    return jax.shard_map(
        on_device,
        mesh=mesh,
        in_specs=(
            P(("fs", "sp"), None), P(), col, col, col, col, col, col,
            P("tp"), P("tp", None), P(("fs", "sp")), P(), P(), P("tp", None), P("tp", None),
        ),
        out_specs=(P(("fs", "sp"), None), P("tp", ("fs", "sp"))),
        check_vma=False,
    )
```
